32 devices in a mesh: grp: 2 (over y), ep: 16 (over z, x, core), tp: 1.
Axes of the slice: x: 2, y: 2, z: 4, core: 2. Of those that a mesh axis runs over, the one named last changes fastest.
Arguments:
- tokens: bfloat16 [2048, 2048], P(('grp', 'ep')), parts along dimension 0, may hold values from -6 to 6
- norm_gain: float32 [2048], replicated, may hold values from 0.1 to 1.9
- routes: int32 [2048, 6], P(('grp', 'ep')), parts along dimension 0, may hold values from 0 to 15, all different within a row; in each aligned block of 64 rows (0 to 63, 64 to 127, ...) at most 48 rows name the same one
- gates: float32 [2048, 6], P(('grp', 'ep')), parts along dimension 0, may hold values from 0.2 to 1
- expert_gate: bfloat16 [16, 2048, 512], P('ep', None, 'tp'), may hold values from -0.125 to 0.125
- expert_up: bfloat16 [16, 2048, 512], P('ep', None, 'tp'), may hold values from -0.125 to 0.125
- expert_down: bfloat16 [16, 512, 2048], P('ep', 'tp'), may hold values from -0.25 to 0.25
- shared_gate: bfloat16 [2048, 512], P(None, 'tp'), may hold values from -0.125 to 0.125
- shared_up: bfloat16 [2048, 512], P(None, 'tp'), may hold values from -0.125 to 0.125
- shared_down: bfloat16 [512, 2048], P('tp'), may hold values from -0.25 to 0.25
Outputs:
- mixed: bfloat16 [2048, 2048], P(('grp', 'ep'), 'tp'), parts along dimension 0
The draws below stay inside these ranges and needn't reach their ends.
There are 2 independent parts, one for each index of `grp`. The reference program is written for one: setup_inputs(seed, part) draws one part's arguments, and reference() takes and returns one part's arrays. A program takes and returns all parts, laid end to end along the dimension named above; an argument that names none is the same for every part. Nothing has to cross between parts.
Inputs may be any that keep to these rules, and one draw needn't show every extreme that they name: `routes`: each row names 6 different experts. In the rows of one index of ep no expert is named by more than 48 rows, and in some such block an expert is named by exactly 48 rows.
All inputs are finite; a program needn't handle non-finite values.
Results may differ from the reference program's by a relative error of at most 0.01.
Values may be sent and summed in bfloat16 or wider, within the bound.
A program may use at most 64 MiB of HBM per device.

```python
import math
import jax
import jax.numpy as jnp
import numpy as np
from jax import lax

D = 2048
FF = 512
SFF = 512
TOP_K = 6
TOK_DEV = 64
EXPERTS = 16
TOKENS = 1024
CAP = 48
N_EP = 16
N_TP = 1


def shard_levels(rng, shape, shards, low, top_value):
    def one(axis_at, parts):
        steps = jax.random.uniform(jax.random.fold_in(jax.random.fold_in(rng, 6), axis_at), (parts,), jnp.float32, low / len(shards), top_value / len(shards))
        return jnp.repeat(jnp.exp(steps), shape[axis_at] // parts).reshape((-1,) + (1,) * (len(shape) - axis_at - 1))

    gain = one(*shards[0])
    for cut in shards[1:]:
        gain = gain * one(*cut)
    return gain


def assign_block(stream_key, own, number, rows, amount, top, most, slope):
    order = jax.random.permutation(stream_key, amount)
    heavy_load, usual = shares(amount, rows * top, most, slope, True), shares(amount, rows * top, most, slope, False)
    places = jnp.arange(amount)

    def named(sizes, rotation):
        used = int((sizes > 0).sum())
        fixed = max(1, used // 4)
        shifted = fixed + (places - fixed + rotation * (used - fixed)) % max(1, amount - fixed)
        return jnp.zeros((amount,), jnp.int32).at[order[jnp.where(places < fixed, places, shifted)]].set(jnp.asarray(sizes, jnp.int32))

    sizes = jnp.where(number % 4 == 0, named(heavy_load, number // 4), named(usual, number - number // 4 - 1))
    mixed = jax.random.permutation(jax.random.fold_in(own, 3), amount)
    giver, receiver = mixed[0:amount // 2 * 2:2], mixed[1:amount // 2 * 2:2]
    room = jnp.minimum(sizes[giver] - 1, most - sizes[receiver]) // 2
    room = jnp.where((giver == order[0]) | (receiver == order[0]) | (sizes[receiver] == 0), 0, jnp.maximum(room, 0))
    shifted = jax.random.randint(jax.random.fold_in(own, 4), (amount // 2,), 0, 1 << 20) % (room + 1)
    sizes = sizes.at[giver].add(-shifted).at[receiver].add(shifted)
    members = jnp.searchsorted(jnp.cumsum(sizes), jnp.arange(rows * top), side="right").astype(jnp.int32)
    grid = members.reshape(top, rows).T
    grid = grid[jax.random.permutation(jax.random.fold_in(own, 1), rows)]
    rotation = jax.random.randint(jax.random.fold_in(own, 2), (rows, 1), 0, top)
    return jnp.take_along_axis(grid, (jnp.arange(top)[None, :] + rotation) % top, axis=1)


def shares(amount, total, most, slope, full):
    portions = [(1 << 20) // math.isqrt(standing ** slope) + 1 for standing in range(1, amount + 1)]
    largest = most if full else min(most, max(-(-total // amount), total * portions[0] // sum(portions)))
    least = 1 if total - largest >= amount - 1 else 0
    holding, surplus = [largest] + [least] * (amount - 1), total - largest - least * (amount - 1)
    while surplus > 0:
        candidates = [i for i in range(1, amount) if holding[i] < largest] or [i for i in range(1, amount) if holding[i] < most]
        whole, remaining = sum([portions[i] for i in candidates]), surplus
        for i in candidates:
            extra = min(most - holding[i], max(1, remaining * portions[i] // whole), surplus)
            holding[i] = holding[i] + extra
            surplus = surplus - extra
    return np.array(holding)


def centred(own_key, dims, scale, reach, cuts=(), held_as=jnp.bfloat16):
    array = scale * jax.random.normal(own_key, dims, jnp.float32)
    if cuts:
        array = array * shard_levels(own_key, dims, cuts, -0.22, 0.18)
    return jnp.clip(array, -reach, reach).astype(held_as)


def setup_inputs(seed: int = 0, part: int = 0) -> dict:
    arg_keys = jax.random.split(jax.random.key(seed), 11)
    part_keys = jax.random.split(jax.random.fold_in(arg_keys[10], part), 11)
    tokens = centred(part_keys[0], (TOKENS, D), 1.0, 6.0, ((0, 16),))
    norm_gain = jnp.clip(1.0 + 0.18 * jax.random.normal(arg_keys[1], (D,), jnp.float32), 0.1, 1.9)
    routes_keys = jax.random.split(jax.random.fold_in(part_keys[2], 1), TOKENS // TOK_DEV)
    routes_turns = jax.random.permutation(jax.random.fold_in(part_keys[2], 3), TOKENS // TOK_DEV)
    routes = jax.vmap(lambda own, number: assign_block(jax.random.fold_in(part_keys[2], 2), own, number, TOK_DEV, EXPERTS, TOP_K, CAP, 2))(routes_keys, routes_turns).reshape((TOKENS, TOP_K))
    gates = jnp.clip(jnp.exp(math.log(1.0) - 1.609438 * jax.random.uniform(part_keys[3], (TOKENS, TOP_K), jnp.float32) ** shard_levels(part_keys[3], (TOKENS, TOP_K), ((0, 16),), -0.2, 0.2)), 0.2, 1.0)
    expert_gate = centred(arg_keys[4], (EXPERTS, D, FF), D ** -0.5, 0.125, ((0, 16),))
    expert_up = centred(arg_keys[5], (EXPERTS, D, FF), D ** -0.5, 0.125, ((0, 16),))
    expert_down = centred(arg_keys[6], (EXPERTS, FF, D), FF ** -0.5, 0.25, ((0, 16),))
    shared_gate = centred(arg_keys[7], (D, SFF), D ** -0.5, 0.125)
    shared_up = centred(arg_keys[8], (D, SFF), D ** -0.5, 0.125)
    shared_down = centred(arg_keys[9], (SFF, D), SFF ** -0.5, 0.25)
    return dict(tokens=tokens, norm_gain=norm_gain, routes=routes, gates=gates, expert_gate=expert_gate, expert_up=expert_up, expert_down=expert_down, shared_gate=shared_gate, shared_up=shared_up, shared_down=shared_down)


def reference(tokens, norm_gain, routes, gates, expert_gate, expert_up, expert_down, shared_gate, shared_up, shared_down):
    values = tokens.astype(jnp.float32)
    scale = lax.rsqrt(lax.optimization_barrier(jnp.mean(values * values, axis=1, keepdims=True)) + 1e-06)
    normed = (values * scale * norm_gain[None, :]).astype(jnp.bfloat16)
    shared_hidden = (jax.nn.silu(jnp.dot(normed, shared_gate, preferred_element_type=jnp.float32)) * jnp.dot(normed, shared_up, preferred_element_type=jnp.float32)).astype(jnp.bfloat16)
    shared_out = jnp.dot(shared_hidden, shared_down, preferred_element_type=jnp.float32)
    bound = N_EP * CAP

    def one_expert(expert, total):
        chosen = routes == expert
        weight = lax.optimization_barrier(jnp.sum(jnp.where(chosen, gates, jnp.float32(0.0)), axis=1))
        live = jnp.any(chosen, axis=1).astype(jnp.int32)
        order = jnp.argsort(1 - live, stable=True)[:bound].astype(jnp.int32)
        rows = normed[order]
        hidden = (jax.nn.silu(jnp.dot(rows, expert_gate[expert], preferred_element_type=jnp.float32)) * jnp.dot(rows, expert_up[expert], preferred_element_type=jnp.float32)).astype(jnp.bfloat16)
        halves = hidden.reshape(bound, N_TP, FF // N_TP).astype(jnp.float32)
        down = expert_down[expert].reshape(N_TP, FF // N_TP, D).astype(jnp.float32)
        partial_value = jnp.einsum('rtf,tfd->trd', halves, down).astype(jnp.bfloat16).astype(jnp.float32)
        result = lax.optimization_barrier(jnp.sum(partial_value, axis=0))
        return total.at[order].add(weight[order][:, None] * result)
    routed = lax.fori_loop(0, EXPERTS, one_expert, jnp.zeros((TOKENS, D), jnp.float32))
    return (routed + shared_out).astype(jnp.bfloat16)
```

```python
import jax
import jax.numpy as jnp
from jax import lax
from jax.sharding import PartitionSpec as P


def expert_rows(rows, w_gate, w_up, w_down):
    hidden = (
        jax.nn.silu(jnp.einsum("...d,df->...f", rows, w_gate, preferred_element_type=jnp.float32))
        * jnp.einsum("...d,df->...f", rows, w_up, preferred_element_type=jnp.float32)
    ).astype(jnp.bfloat16)
    return jnp.einsum("...f,fd->...d", hidden, w_down, preferred_element_type=jnp.float32).astype(
        jnp.bfloat16
    )


def run_experts(received, ranks, local_experts, expert_gate, expert_up, expert_down):
    count = received.shape[1]
    cols = received.shape[2]
    grouped = received.reshape(ranks, local_experts, count, cols)
    results = jnp.stack(
        [expert_rows(grouped[:, 0], expert_gate[0], expert_up[0], expert_down[0])], axis=1
    )
    return results.reshape(ranks * local_experts, count, results.shape[-1])


def shards(
    tokens,
    norm_gain,
    routes,
    gates,
    expert_gate,
    expert_up,
    expert_down,
    shared_gate,
    shared_up,
    shared_down,
):
    rows_here = tokens.shape[0]
    picks = routes.shape[1]
    local_experts = expert_gate.shape[0]
    ranks = lax.axis_size("ep")
    all_experts = local_experts * ranks
    capacity = max(2, min(rows_here, 2 * rows_here * picks // all_experts))
    values = tokens.astype(jnp.float32)
    scale = lax.rsqrt(jnp.mean(values * values, axis=1, keepdims=True) + 1e-06)
    normed = (values * scale * norm_gain[None, :]).astype(jnp.bfloat16)
    shared_hidden = (
        jax.nn.silu(jnp.dot(normed, shared_gate, preferred_element_type=jnp.float32))
        * jnp.dot(normed, shared_up, preferred_element_type=jnp.float32)
    ).astype(jnp.bfloat16)
    shared_out = jnp.dot(shared_hidden, shared_down, preferred_element_type=jnp.float32)
    flat = routes.reshape(-1)
    matches = (flat[:, None] == jnp.arange(all_experts, dtype=jnp.int32)[None, :]).astype(jnp.int32)
    earlier = jnp.cumsum(matches, axis=0) - matches
    slots = jnp.sum(earlier * matches, axis=1)
    target = flat * capacity + slots
    picker = target[None, :] == jnp.arange(all_experts * capacity, dtype=jnp.int32)[:, None]
    picker = picker.reshape(all_experts * capacity, rows_here, picks)
    take_rows = jnp.any(picker, axis=2).astype(jnp.bfloat16)
    buffer = jnp.dot(take_rows, normed, preferred_element_type=jnp.float32).astype(jnp.bfloat16)
    buffer = buffer.reshape(all_experts, capacity, normed.shape[1])
    results = run_experts(
        lax.all_to_all(buffer, "ep", split_axis=0, concat_axis=0, tiled=True),
        ranks,
        local_experts,
        expert_gate,
        expert_up,
        expert_down,
    )
    returned = lax.all_to_all(results, "ep", split_axis=0, concat_axis=0, tiled=True)
    flat_back = returned.reshape(all_experts * capacity, returned.shape[2])
    picked = flat_back[target].reshape(rows_here, picks, returned.shape[2]).astype(jnp.float32)
    routed = jnp.sum(gates[:, :, None] * picked, axis=1)
    payload = routed + shared_out
    summed = lax.psum_scatter(payload.astype(jnp.bfloat16), "tp", scatter_dimension=1, tiled=True)
    return summed


def dense_shards(
    tokens,
    norm_gain,
    routes,
    gates,
    expert_gate,
    expert_up,
    expert_down,
    shared_gate,
    shared_up,
    shared_down,
):
    cols = tokens.shape[1]
    experts = lax.axis_size("ep")
    me = lax.axis_index("ep")
    values = tokens.astype(jnp.float32)
    scale = lax.rsqrt(jnp.mean(values * values, axis=1, keepdims=True) + 1e-06)
    normed = (values * scale * norm_gain[None, :]).astype(jnp.bfloat16)
    lanes = jnp.arange(experts, dtype=jnp.int32)
    weight = jnp.sum(
        jnp.where(routes[:, :, None] == lanes[None, None, :], gates[:, :, None], 0.0), axis=1
    )
    high = weight.astype(jnp.bfloat16)
    low = (weight - high.astype(jnp.float32)).astype(jnp.bfloat16)
    gathered = lax.all_gather(
        jnp.concatenate([normed, high, low], axis=1), "ep", axis=0, tiled=True
    )
    tail = gathered[:, cols:].astype(jnp.float32)
    places = jnp.arange(2 * experts, dtype=jnp.int32)
    mine = jnp.sum(jnp.where((places % experts == me)[None, :], tail, 0.0), axis=1, keepdims=True)
    rows = gathered[:, :cols]
    hidden = (
        jax.nn.silu(jnp.dot(rows, expert_gate[0], preferred_element_type=jnp.float32))
        * jnp.dot(rows, expert_up[0], preferred_element_type=jnp.float32)
    ).astype(jnp.bfloat16)
    partial = jnp.dot(hidden, expert_down[0], preferred_element_type=jnp.float32)
    shared_hidden = (
        jax.nn.silu(jnp.dot(normed, shared_gate, preferred_element_type=jnp.float32))
        * jnp.dot(normed, shared_up, preferred_element_type=jnp.float32)
    ).astype(jnp.bfloat16)
    shared_out = jnp.dot(shared_hidden, shared_down, preferred_element_type=jnp.float32)
    routed = lax.psum_scatter(
        (partial * mine).astype(jnp.bfloat16), "ep", scatter_dimension=0, tiled=True
    )
    return (routed.astype(jnp.float32) + shared_out).astype(jnp.bfloat16)


def solution(mesh):
    in_specs = (
        P(("grp", "ep"), None),
        P(),
        P(("grp", "ep"), None),
        P(("grp", "ep"), None),
        P("ep", None, "tp"),
        P("ep", None, "tp"),
        P("ep", "tp", None),
        P(None, "tp"),
        P(None, "tp"),
        P("tp", None),
    )
    out_specs = P(("grp", "ep"), "tp")
    body = dense_shards if mesh.shape['tp'] == 1 else shards
    return jax.shard_map(body, mesh=mesh, in_specs=in_specs, out_specs=out_specs, check_vma=False)
```

```python
import functools

import jax
import jax.numpy as jnp
from jax import lax
from jax.experimental import pallas as pl
from jax.experimental.pallas import tpu as pltpu
from jax.sharding import PartitionSpec as P


def expert_rows(rows, w_gate, w_up, w_down):
    hidden = (
        jax.nn.silu(jnp.einsum("...d,df->...f", rows, w_gate, preferred_element_type=jnp.float32))
        * jnp.einsum("...d,df->...f", rows, w_up, preferred_element_type=jnp.float32)
    ).astype(jnp.bfloat16)
    return jnp.einsum("...f,fd->...d", hidden, w_down, preferred_element_type=jnp.float32).astype(
        jnp.bfloat16
    )


def run_experts(received, ranks, local_experts, expert_gate, expert_up, expert_down):
    count = received.shape[1]
    cols = received.shape[2]
    grouped = received.reshape(ranks, local_experts, count, cols)
    results = jnp.stack(
        [expert_rows(grouped[:, 0], expert_gate[0], expert_up[0], expert_down[0])], axis=1
    )
    return results.reshape(ranks * local_experts, count, results.shape[-1])


def shards(
    tokens,
    norm_gain,
    routes,
    gates,
    expert_gate,
    expert_up,
    expert_down,
    shared_gate,
    shared_up,
    shared_down,
):
    rows_here = tokens.shape[0]
    picks = routes.shape[1]
    local_experts = expert_gate.shape[0]
    ranks = lax.axis_size("ep")
    all_experts = local_experts * ranks
    capacity = max(2, min(rows_here, 2 * rows_here * picks // all_experts))
    values = tokens.astype(jnp.float32)
    scale = lax.rsqrt(jnp.mean(values * values, axis=1, keepdims=True) + 1e-06)
    normed = (values * scale * norm_gain[None, :]).astype(jnp.bfloat16)
    shared_hidden = (
        jax.nn.silu(jnp.dot(normed, shared_gate, preferred_element_type=jnp.float32))
        * jnp.dot(normed, shared_up, preferred_element_type=jnp.float32)
    ).astype(jnp.bfloat16)
    shared_out = jnp.dot(shared_hidden, shared_down, preferred_element_type=jnp.float32)
    flat = routes.reshape(-1)
    matches = (flat[:, None] == jnp.arange(all_experts, dtype=jnp.int32)[None, :]).astype(jnp.int32)
    earlier = jnp.cumsum(matches, axis=0) - matches
    slots = jnp.sum(earlier * matches, axis=1)
    target = flat * capacity + slots
    picker = target[None, :] == jnp.arange(all_experts * capacity, dtype=jnp.int32)[:, None]
    picker = picker.reshape(all_experts * capacity, rows_here, picks)
    take_rows = jnp.any(picker, axis=2).astype(jnp.bfloat16)
    buffer = jnp.dot(take_rows, normed, preferred_element_type=jnp.float32).astype(jnp.bfloat16)
    buffer = buffer.reshape(all_experts, capacity, normed.shape[1])
    results = run_experts(
        lax.all_to_all(buffer, "ep", split_axis=0, concat_axis=0, tiled=True),
        ranks,
        local_experts,
        expert_gate,
        expert_up,
        expert_down,
    )
    returned = lax.all_to_all(results, "ep", split_axis=0, concat_axis=0, tiled=True)
    flat_back = returned.reshape(all_experts * capacity, returned.shape[2])
    picked = flat_back[target].reshape(rows_here, picks, returned.shape[2]).astype(jnp.float32)
    routed = jnp.sum(gates[:, :, None] * picked, axis=1)
    payload = routed + shared_out
    summed = lax.psum_scatter(payload.astype(jnp.bfloat16), "tp", scatter_dimension=1, tiled=True)
    return summed


def fused_kernel(
    nz,
    pieces,
    tokens,
    gain,
    routes,
    gates,
    eg_hbm,
    eu_hbm,
    ed_hbm,
    sg_hbm,
    su_hbm,
    sd_hbm,
    out,
    ag,
    eg,
    eu,
    ed,
    sg,
    su,
    sd,
    shared,
    keep,
    psend,
    rs_d,
    sx,
    rs_x,
    sz,
    chain,
    wsem,
    z_send,
    z_recv,
    x_send,
    x_recv,
    d_send,
    d_recv,
    rd_send,
    rd_recv,
    rx_send,
    rx_recv,
    rz_send,
    rz_recv,
):
    rows, cols = tokens.shape
    experts = 4 * nz
    me = lax.axis_index("ep")
    z, x, c = me // 4, (me // 2) % 2, me % 2
    partner = 4 * z + 2 * x + (1 - c)
    across = 4 * z + 2 * (1 - x) + c
    up, down = jnp.minimum(z + 1, nz - 1) * 4 + 2 * x + c, jnp.maximum(z - 1, 0) * 4 + 2 * x + c

    loads = [
        pltpu.make_async_copy(src, dst, wsem.at[i])
        for i, (src, dst) in enumerate(
            [(sg_hbm, sg), (su_hbm, su), (sd_hbm, sd), (eg_hbm, eg), (eu_hbm, eu), (ed_hbm, ed)]
        )
    ]
    for load in loads:
        load.start()

    def remote(src, dst, send, recv, to):
        return pltpu.make_async_remote_copy(
            src_ref=src,
            dst_ref=dst,
            send_sem=send,
            recv_sem=recv,
            device_id={"ep": to},
            device_id_type=pl.DeviceIdType.MESH,
        )

    def part(p, rc, rx):
        start, size, _ = pieces[p]
        return pl.ds((rc * 2 + rx) * rows + start, size)

    def ag_z(layer, rx, p, way):
        ref = ag.at[layer, part(p, 0, rx)]
        to = up if way == 0 else down
        return remote(ref, ref, z_send.at[way, layer, rx, p], z_recv.at[layer, rx, p], to)

    def ag_x(layer, p):
        return remote(
            ag.at[layer, part(p, 0, 0)],
            ag.at[layer, part(p, 0, 1)],
            x_send.at[layer, p],
            x_recv.at[layer, p],
            across,
        )

    def ag_d(layer, rx, p):
        return remote(
            ag.at[layer, part(p, 0, rx)],
            ag.at[layer, part(p, 1, rx)],
            d_send.at[layer, rx, p],
            d_recv.at[layer, rx, p],
            partner,
        )

    def rs_core(layer):
        return remote(
            psend.at[layer], rs_d.at[layer], rd_send.at[layer], rd_recv.at[layer], partner
        )

    def rs_across(layer, p):
        ds = part(p, 0, 0)
        return remote(
            sx.at[layer, ds], rs_x.at[layer, ds], rx_send.at[layer, p], rx_recv.at[layer, p], across
        )

    def rs_z(layer, rx, p, way):
        ds = part(p, 0, rx)
        to = up if way == 0 else down
        return remote(
            sz.at[layer, ds],
            chain.at[way, layer, ds],
            rz_send.at[layer, rx, p],
            rz_recv.at[way, layer, rx, p],
            to,
        )

    count = range(len(pieces))
    kinds = [(p, rx) for p in count for rx in ((0, 1) if pieces[p][2] else (0,))]

    def has(way):
        return z < nz - 1 if way == 0 else z > 0

    barrier = pltpu.get_barrier_semaphore()
    for to in (partner, across):
        pl.semaphore_signal(
            barrier, inc=1, device_id={"ep": to}, device_id_type=pl.DeviceIdType.MESH
        )
    for way, to in ((0, up), (1, down)):

        @pl.when(has(way))
        def _():
            pl.semaphore_signal(
                barrier, inc=1, device_id={"ep": to}, device_id_type=pl.DeviceIdType.MESH
            )

    values = tokens[...].astype(jnp.float32)
    scale = lax.rsqrt(jnp.mean(values * values, axis=1, keepdims=True) + 1e-06)
    normed = (values * scale * gain[...]).astype(jnp.bfloat16)
    width = ag.shape[2] - cols
    lane = lax.broadcasted_iota(jnp.int32, (rows, width), 1)
    expert = lane % experts
    weight = jnp.zeros((rows, width), jnp.float32)
    for k in range(routes.shape[1]):
        weight += jnp.where(expert == routes[:, k : k + 1], gates[:, k : k + 1], 0.0)
    high = weight.astype(jnp.bfloat16).astype(jnp.float32)
    tail = jnp.where(lane < experts, high, jnp.where(lane < 2 * experts, weight - high, 0.0))
    ag[z, :rows, :cols] = normed
    ag[z, :rows, cols:] = tail.astype(jnp.bfloat16)

    peers = 2 + jnp.minimum(z, 1) + jnp.minimum(nz - 1 - z, 1)
    pl.semaphore_wait(barrier, peers)

    for p in sorted(count, key=lambda p: not pieces[p][2]):
        ag_x(z, p).start()
        for way in (0, 1):

            @pl.when(has(way))
            def _():
                ag_z(z, 0, p, way).start()

        ag_d(z, 0, p).start()

    for load in loads[:3]:
        load.wait()
    mine = ag[z, :rows, :cols]
    gate = jnp.dot(mine, sg[...], preferred_element_type=jnp.float32)
    lift = jnp.dot(mine, su[...], preferred_element_type=jnp.float32)
    hidden = (jax.nn.silu(gate) * lift).astype(jnp.bfloat16)
    shared[...] = jnp.dot(hidden, sd[...], preferred_element_type=jnp.float32)

    for p in sorted(count, key=lambda p: not pieces[p][2]):
        ag_x(z, p).wait_recv()
        ag_d(z, 1, p).start()
        if pieces[p][2]:
            for way in (0, 1):

                @pl.when(has(way))
                def _():
                    ag_z(z, 1, p, way).start()

    for load in loads[3:]:
        load.wait()

    def at_distance(d, body):
        for way, layer, inside in ((0, z - d, z - d >= 0), (1, z + d, z + d < nz)):

            @pl.when(inside)
            def _():
                body(layer, way)

    def forward(layer, way):
        for p, rx in kinds:
            ag_z(layer, rx, p, way).wait_recv()

            @pl.when(has(way))
            def _():
                ag_z(layer, rx, p, way).start()

            if not pieces[p][2]:
                ag_x(layer, p).start()
            ag_d(layer, rx, p).start()

    def relay(layer, way):
        for p in count:
            if not pieces[p][2]:
                ag_x(layer, p).wait_recv()
                ag_d(layer, 1, p).start()

    def pick(table, k):
        found = 0
        for i, line in enumerate(table):
            for j, layer in enumerate(line):
                found = jnp.where(jnp.logical_and(z == i, k == j), layer, found)
        return found

    inner = [
        list(range(i + 1, nz)) + list(range(i - 1, -1, -1))
        if 2 * i < nz
        else list(range(i - 1, -1, -1)) + list(range(i + 1, nz))
        for i in range(nz)
    ]
    order = [
        [i] + sorted(inner[i], key=lambda layer: abs(layer - i)) for i in range(nz)
    ]

    def experts_on(layer):
        for p in count:
            for rx in (0, 1):
                ag_d(layer, rx, p).wait_recv()
        block = ag[layer, :, :cols]
        tails = ag[layer, :, cols:].astype(jnp.float32)
        spot = lax.broadcasted_iota(jnp.int32, tails.shape, 1) % experts
        share = jnp.sum(jnp.where(spot == me, tails, 0.0), axis=1, keepdims=True)
        a = jnp.dot(block, eg[...], preferred_element_type=jnp.float32)
        b = jnp.dot(block, eu[...], preferred_element_type=jnp.float32)
        h = (jax.nn.silu(a) * b).astype(jnp.bfloat16)
        step = cols // 4
        for i in range(4):
            cs = slice(i * step, (i + 1) * step)
            y = jnp.dot(h, ed[:, cs], preferred_element_type=jnp.float32) * share
            keep[layer, :, cs] = y[: 2 * rows]
            psend[layer, :, cs] = y[2 * rows :].astype(jnp.bfloat16)
        rs_core(layer).start()

    def fold_core(layer):
        rs_core(layer).wait_recv()
        for p in count:
            if not pieces[p][2]:
                ds = part(p, 0, 1)
                both = keep[layer, ds] + rs_d[layer, ds].astype(jnp.float32)
                sx[layer, part(p, 0, 0)] = both.astype(jnp.bfloat16)
                rs_across(layer, p).start()

    def local_sum(layer, rx, p):
        ds = part(p, 0, rx)
        total = keep[layer, ds] + rs_d[layer, ds].astype(jnp.float32)
        if not pieces[p][2]:
            total += rs_x[layer, ds].astype(jnp.float32)
        return total

    def send_sum(layer):
        for way in (0, 1):
            arrives = z > 0 if way == 0 else z < nz - 1

            @pl.when(layer > z if way == 0 else layer < z)
            def _():
                for p, rx in kinds:
                    ds = part(p, 0, rx)
                    if not pieces[p][2]:
                        rs_across(layer, p).wait_recv()

                    @pl.when(arrives)
                    def _():
                        rs_z(layer, rx, p, way).wait_recv()
                        more = chain[way, layer, ds].astype(jnp.float32)
                        sz[layer, ds] = (local_sum(layer, rx, p) + more).astype(jnp.bfloat16)

                    @pl.when(jnp.logical_not(arrives))
                    def _():
                        sz[layer, ds] = local_sum(layer, rx, p).astype(jnp.bfloat16)

                    rs_z(layer, rx, p, way).start()

    edge = jnp.logical_or(z == 0, z == nz - 1)

    @pl.loop(0, nz)
    def _(k):
        at_distance(k + 1, forward)
        experts_on(pick(order, k))
        at_distance(k + 1, relay)

        @pl.when(k >= 1)
        def _():
            fold_core(pick(order, k - 1))

        @pl.when(jnp.logical_and(k >= 2, edge))
        def _():
            send_sum(pick(order, k - 1))

    fold_core(pick(order, nz - 1))

    @pl.loop(0, nz - 1)
    def _(j):
        @pl.when(jnp.logical_or(jnp.logical_not(edge), j == nz - 2))
        def _():
            send_sum(pick(inner, j))

    def add_chains(p, rx):
        ds = part(p, 0, rx)
        for way in (0, 1):

            @pl.when(z > 0 if way == 0 else z < nz - 1)
            def _():
                rs_z(z, rx, p, way).wait_recv()
                keep[z, ds] = keep[z, ds] + chain[way, z, ds].astype(jnp.float32)

    for p in count:
        if pieces[p][2]:
            add_chains(p, 1)
            sx[z, part(p, 0, 0)] = local_sum(z, 1, p).astype(jnp.bfloat16)
            rs_across(z, p).start()
    for p in sorted(count, key=lambda p: pieces[p][2]):
        ds = part(p, 0, 0)
        add_chains(p, 0)
        rs_across(z, p).wait_recv()
        total = local_sum(z, 0, p) + shared[ds]
        if pieces[p][2]:
            total += rs_x[z, ds].astype(jnp.float32)
        out[ds] = total.astype(out.dtype)

    @pl.loop(0, nz)
    def _(layer):
        for p in count:
            for rx in (0, 1):
                ag_d(layer, rx, p).wait_send()
            if not pieces[p][2]:
                ag_x(layer, p).wait_send()
                rs_across(layer, p).wait_send()
            else:

                @pl.when(layer == z)
                def _():
                    ag_x(layer, p).wait_send()
                    rs_across(layer, p).wait_send()

        rs_core(layer).wait_send()
        for way in (0, 1):
            behind = layer <= z if way == 0 else layer >= z
            ahead = layer > z if way == 0 else layer < z

            @pl.when(jnp.logical_and(behind, has(way)))
            def _():
                for p, rx in kinds:
                    ag_z(layer, rx, p, way).wait_send()

            @pl.when(ahead)
            def _():
                for p, rx in kinds:
                    rs_z(layer, rx, p, way).wait_send()


def fused_shards(
    tokens,
    norm_gain,
    routes,
    gates,
    expert_gate,
    expert_up,
    expert_down,
    shared_gate,
    shared_up,
    shared_down,
):
    rows, cols = tokens.shape
    ff = expert_gate.shape[2]
    shared_ff = shared_gate.shape[1]
    ranks = lax.axis_size("ep")
    nz = ranks // 4
    pieces = make_pieces(rows)
    count = len(pieces)
    width = cols + -(-2 * ranks // 128) * 128
    half, narrow = jnp.bfloat16, pltpu.SemaphoreType.DMA
    vmem, anywhere = pl.BlockSpec(memory_space=pltpu.VMEM), pl.BlockSpec(memory_space=pl.ANY)
    return pl.pallas_call(
        functools.partial(fused_kernel, nz, pieces),
        out_shape=jax.ShapeDtypeStruct((rows, cols), half),
        in_specs=[vmem] * 4 + [anywhere] * 6,
        out_specs=vmem,
        scratch_shapes=[
            pltpu.VMEM((nz, 4 * rows, width), half),
            pltpu.VMEM((cols, ff), half),
            pltpu.VMEM((cols, ff), half),
            pltpu.VMEM((ff, cols), half),
            pltpu.VMEM((cols, shared_ff), half),
            pltpu.VMEM((cols, shared_ff), half),
            pltpu.VMEM((shared_ff, cols), half),
            pltpu.VMEM((rows, cols), jnp.float32),
            pltpu.VMEM((nz, 2 * rows, cols), jnp.float32),
            pltpu.VMEM((nz, 2 * rows, cols), half),
            pltpu.VMEM((nz, 2 * rows, cols), half),
            pltpu.VMEM((nz, rows, cols), half),
            pltpu.VMEM((nz, rows, cols), half),
            pltpu.VMEM((nz, 2 * rows, cols), half),
            pltpu.VMEM((2, nz, 2 * rows, cols), half),
            narrow((6,)),
            narrow((2, nz, 2, count)),
            narrow((nz, 2, count)),
            narrow((nz, count)),
            narrow((nz, count)),
            narrow((nz, 2, count)),
            narrow((nz, 2, count)),
            narrow((nz,)),
            narrow((nz,)),
            narrow((nz, count)),
            narrow((nz, count)),
            narrow((nz, 2, count)),
            narrow((2, nz, 2, count)),
        ],
        compiler_params=pltpu.CompilerParams(
            collective_id=0, has_side_effects=True, vmem_limit_bytes=60 * 1024 * 1024
        ),
    )(
        tokens,
        norm_gain[None, :],
        routes,
        gates,
        expert_gate[0],
        expert_up[0],
        expert_down[0],
        shared_gate,
        shared_up,
        shared_down,
    )


def make_pieces(rows):
    unit = rows // 4
    return [(0, 2 * unit, False), (2 * unit, unit, False), (3 * unit, unit, True)]


def solution(mesh):
    in_specs = (
        P(("grp", "ep"), None),
        P(),
        P(("grp", "ep"), None),
        P(("grp", "ep"), None),
        P("ep", None, "tp"),
        P("ep", None, "tp"),
        P("ep", "tp", None),
        P(None, "tp"),
        P(None, "tp"),
        P("tp", None),
    )
    out_specs = P(("grp", "ep"), "tp")
    def body(*args):
        fits = mesh.shape["tp"] == 1 and mesh.shape["ep"] % 4 == 0 and args[4].shape[0] == 1
        small = args[0].shape[0] * mesh.shape["ep"] <= args[4].shape[1]
        return (fused_shards if fits and small else shards)(*args)

    return jax.shard_map(body, mesh=mesh, in_specs=in_specs, out_specs=out_specs, check_vma=False)
```

```python
import functools

import jax
import jax.numpy as jnp
from jax import lax
from jax.experimental import pallas as pl
from jax.experimental.pallas import tpu as pltpu
from jax.sharding import PartitionSpec as P


def expert_rows(rows, w_gate, w_up, w_down):
    hidden = (
        jax.nn.silu(jnp.einsum("...d,df->...f", rows, w_gate, preferred_element_type=jnp.float32))
        * jnp.einsum("...d,df->...f", rows, w_up, preferred_element_type=jnp.float32)
    ).astype(jnp.bfloat16)
    return jnp.einsum("...f,fd->...d", hidden, w_down, preferred_element_type=jnp.float32).astype(
        jnp.bfloat16
    )


def run_experts(received, ranks, local_experts, expert_gate, expert_up, expert_down):
    count = received.shape[1]
    cols = received.shape[2]
    grouped = received.reshape(ranks, local_experts, count, cols)
    results = jnp.stack(
        [expert_rows(grouped[:, 0], expert_gate[0], expert_up[0], expert_down[0])], axis=1
    )
    return results.reshape(ranks * local_experts, count, results.shape[-1])


def shards(
    tokens,
    norm_gain,
    routes,
    gates,
    expert_gate,
    expert_up,
    expert_down,
    shared_gate,
    shared_up,
    shared_down,
):
    rows_here = tokens.shape[0]
    picks = routes.shape[1]
    local_experts = expert_gate.shape[0]
    ranks = lax.axis_size("ep")
    all_experts = local_experts * ranks
    capacity = max(2, min(rows_here, 2 * rows_here * picks // all_experts))
    values = tokens.astype(jnp.float32)
    scale = lax.rsqrt(jnp.mean(values * values, axis=1, keepdims=True) + 1e-06)
    normed = (values * scale * norm_gain[None, :]).astype(jnp.bfloat16)
    shared_hidden = (
        jax.nn.silu(jnp.dot(normed, shared_gate, preferred_element_type=jnp.float32))
        * jnp.dot(normed, shared_up, preferred_element_type=jnp.float32)
    ).astype(jnp.bfloat16)
    shared_out = jnp.dot(shared_hidden, shared_down, preferred_element_type=jnp.float32)
    flat = routes.reshape(-1)
    matches = (flat[:, None] == jnp.arange(all_experts, dtype=jnp.int32)[None, :]).astype(jnp.int32)
    earlier = jnp.cumsum(matches, axis=0) - matches
    slots = jnp.sum(earlier * matches, axis=1)
    target = flat * capacity + slots
    picker = target[None, :] == jnp.arange(all_experts * capacity, dtype=jnp.int32)[:, None]
    picker = picker.reshape(all_experts * capacity, rows_here, picks)
    take_rows = jnp.any(picker, axis=2).astype(jnp.bfloat16)
    buffer = jnp.dot(take_rows, normed, preferred_element_type=jnp.float32).astype(jnp.bfloat16)
    buffer = buffer.reshape(all_experts, capacity, normed.shape[1])
    results = run_experts(
        lax.all_to_all(buffer, "ep", split_axis=0, concat_axis=0, tiled=True),
        ranks,
        local_experts,
        expert_gate,
        expert_up,
        expert_down,
    )
    returned = lax.all_to_all(results, "ep", split_axis=0, concat_axis=0, tiled=True)
    flat_back = returned.reshape(all_experts * capacity, returned.shape[2])
    picked = flat_back[target].reshape(rows_here, picks, returned.shape[2]).astype(jnp.float32)
    routed = jnp.sum(gates[:, :, None] * picked, axis=1)
    payload = routed + shared_out
    summed = lax.psum_scatter(payload.astype(jnp.bfloat16), "tp", scatter_dimension=1, tiled=True)
    return summed


def fused_kernel(
    nz,
    pieces,
    tokens,
    gain,
    routes,
    gates,
    eg_hbm,
    eu_hbm,
    ed_hbm,
    sg_hbm,
    su_hbm,
    sd_hbm,
    out,
    ag,
    eg,
    eu,
    ed,
    sg,
    su,
    sd,
    shared,
    keep,
    psend,
    rs_d,
    sx,
    rs_x,
    sz,
    chain,
    wsem,
    z_send,
    z_recv,
    x_send,
    x_recv,
    d_send,
    d_recv,
    rd_send,
    rd_recv,
    rx_send,
    rx_recv,
    rz_send,
    rz_recv,
):
    rows, cols = tokens.shape
    experts = 4 * nz
    me = lax.axis_index("ep")
    z, x, c = me // 4, (me // 2) % 2, me % 2
    partner = 4 * z + 2 * x + (1 - c)
    across = 4 * z + 2 * (1 - x) + c
    up, down = jnp.minimum(z + 1, nz - 1) * 4 + 2 * x + c, jnp.maximum(z - 1, 0) * 4 + 2 * x + c

    loads = [
        pltpu.make_async_copy(src, dst, wsem.at[i])
        for i, (src, dst) in enumerate(
            [(sg_hbm, sg), (su_hbm, su), (sd_hbm, sd), (eg_hbm, eg), (eu_hbm, eu), (ed_hbm, ed)]
        )
    ]
    for load in loads:
        load.start()

    def remote(src, dst, send, recv, to):
        return pltpu.make_async_remote_copy(
            src_ref=src,
            dst_ref=dst,
            send_sem=send,
            recv_sem=recv,
            device_id={"ep": to},
            device_id_type=pl.DeviceIdType.MESH,
        )

    def part(p, rc, rx):
        start, size, _ = pieces[p]
        return pl.ds((rc * 2 + rx) * rows + start, size)

    def ag_z(layer, rx, p, way):
        ref = ag.at[layer, part(p, 0, rx)]
        to = up if way == 0 else down
        return remote(ref, ref, z_send.at[way, layer, rx, p], z_recv.at[layer, rx, p], to)

    def ag_x(layer, p):
        return remote(
            ag.at[layer, part(p, 0, 0)],
            ag.at[layer, part(p, 0, 1)],
            x_send.at[layer, p],
            x_recv.at[layer, p],
            across,
        )

    def ag_d(layer, rx, p):
        return remote(
            ag.at[layer, part(p, 0, rx)],
            ag.at[layer, part(p, 1, rx)],
            d_send.at[layer, rx, p],
            d_recv.at[layer, rx, p],
            partner,
        )

    def rs_core(layer):
        return remote(
            psend.at[layer], rs_d.at[layer], rd_send.at[layer], rd_recv.at[layer], partner
        )

    def rs_across(layer, p):
        ds = part(p, 0, 0)
        return remote(
            sx.at[layer, ds], rs_x.at[layer, ds], rx_send.at[layer, p], rx_recv.at[layer, p], across
        )

    def rs_z(layer, rx, p, way):
        ds = part(p, 0, rx)
        to = up if way == 0 else down
        return remote(
            sz.at[layer, ds],
            chain.at[way, layer, ds],
            rz_send.at[layer, rx, p],
            rz_recv.at[way, layer, rx, p],
            to,
        )

    count = range(len(pieces))
    kinds = [(p, rx) for p in count for rx in ((0, 1) if pieces[p][2] else (0,))]

    def has(way):
        return z < nz - 1 if way == 0 else z > 0

    barrier = pltpu.get_barrier_semaphore()
    for to in (partner, across):
        pl.semaphore_signal(
            barrier, inc=1, device_id={"ep": to}, device_id_type=pl.DeviceIdType.MESH
        )
    for way, to in ((0, up), (1, down)):

        @pl.when(has(way))
        def _():
            pl.semaphore_signal(
                barrier, inc=1, device_id={"ep": to}, device_id_type=pl.DeviceIdType.MESH
            )

    values = tokens[...].astype(jnp.float32)
    scale = lax.rsqrt(jnp.mean(values * values, axis=1, keepdims=True) + 1e-06)
    normed = (values * scale * gain[...]).astype(jnp.bfloat16)
    width = ag.shape[2] - cols
    spots = lax.broadcasted_iota(jnp.int32, (width, rows), 0)
    expert = spots % experts
    weight = jnp.zeros((width, rows), jnp.float32)
    for k in range(routes.shape[0]):
        weight += jnp.where(expert == routes[k : k + 1, :], gates[k : k + 1, :], 0.0)
    high = weight.astype(jnp.bfloat16).astype(jnp.float32)
    tail = jnp.where(spots < experts, high, jnp.where(spots < 2 * experts, weight - high, 0.0)).T
    ag[z, :rows, :cols] = normed
    ag[z, :rows, cols:] = tail.astype(jnp.bfloat16)

    peers = 2 + jnp.minimum(z, 1) + jnp.minimum(nz - 1 - z, 1)
    pl.semaphore_wait(barrier, peers)

    for p in sorted(count, key=lambda p: not pieces[p][2]):
        ag_x(z, p).start()
        for way in (0, 1):

            @pl.when(has(way))
            def _():
                ag_z(z, 0, p, way).start()

        ag_d(z, 0, p).start()

    for p in sorted(count, key=lambda p: not pieces[p][2]):
        ag_x(z, p).wait_recv()
        ag_d(z, 1, p).start()
        if pieces[p][2]:
            for way in (0, 1):

                @pl.when(has(way))
                def _():
                    ag_z(z, 1, p, way).start()

    def at_distance(d, body):
        for way, layer, inside in ((0, z - d, z - d >= 0), (1, z + d, z + d < nz)):

            @pl.when(inside)
            def _():
                body(layer, way)

    def forward(layer, way):
        for p, rx in kinds:
            ag_z(layer, rx, p, way).wait_recv()

            @pl.when(has(way))
            def _():
                ag_z(layer, rx, p, way).start()

            if not pieces[p][2]:
                ag_x(layer, p).start()
            ag_d(layer, rx, p).start()

    def relay(layer, way):
        for p in count:
            if not pieces[p][2]:
                ag_x(layer, p).wait_recv()
                ag_d(layer, 1, p).start()

    def pick(table, k):
        found = 0
        for i, line in enumerate(table):
            for j, layer in enumerate(line):
                found = jnp.where(jnp.logical_and(z == i, k == j), layer, found)
        return found

    inner = [
        list(range(i + 1, nz)) + list(range(i - 1, -1, -1))
        if 2 * i < nz
        else list(range(i - 1, -1, -1)) + list(range(i + 1, nz))
        for i in range(nz)
    ]
    order = [
        [i] + sorted(inner[i], key=lambda layer: abs(layer - i)) for i in range(nz)
    ]

    def experts_on(layer):
        for p in count:
            for rx in (0, 1):
                ag_d(layer, rx, p).wait_recv()
        block = ag[layer, :, :cols]
        tails = ag[layer, :, cols:].astype(jnp.float32)
        spot = lax.broadcasted_iota(jnp.int32, tails.shape, 1) % experts
        share = jnp.sum(jnp.where(spot == me, tails, 0.0), axis=1, keepdims=True)
        a = jnp.dot(block, eg[...], preferred_element_type=jnp.float32)
        b = jnp.dot(block, eu[...], preferred_element_type=jnp.float32)
        h = (jax.nn.silu(a) * b).astype(jnp.bfloat16)
        step = cols // 4
        for i in range(4):
            cs = slice(i * step, (i + 1) * step)
            y = jnp.dot(h, ed[:, cs], preferred_element_type=jnp.float32) * share
            keep[layer, :, cs] = y[: 2 * rows]
            psend[layer, :, cs] = y[2 * rows :].astype(jnp.bfloat16)
        rs_core(layer).start()

    def fold_core(layer):
        rs_core(layer).wait_recv()
        for p in count:
            if not pieces[p][2]:
                ds = part(p, 0, 1)
                both = keep[layer, ds] + rs_d[layer, ds].astype(jnp.float32)
                sx[layer, part(p, 0, 0)] = both.astype(jnp.bfloat16)
                rs_across(layer, p).start()

    def local_sum(layer, rx, p):
        ds = part(p, 0, rx)
        total = keep[layer, ds] + rs_d[layer, ds].astype(jnp.float32)
        if not pieces[p][2]:
            total += rs_x[layer, ds].astype(jnp.float32)
        return total

    def send_sum(layer):
        for way in (0, 1):
            arrives = z > 0 if way == 0 else z < nz - 1

            @pl.when(layer > z if way == 0 else layer < z)
            def _():
                for p, rx in kinds:
                    ds = part(p, 0, rx)
                    if not pieces[p][2]:
                        rs_across(layer, p).wait_recv()

                    @pl.when(arrives)
                    def _():
                        rs_z(layer, rx, p, way).wait_recv()
                        more = chain[way, layer, ds].astype(jnp.float32)
                        sz[layer, ds] = (local_sum(layer, rx, p) + more).astype(jnp.bfloat16)

                    @pl.when(jnp.logical_not(arrives))
                    def _():
                        sz[layer, ds] = local_sum(layer, rx, p).astype(jnp.bfloat16)

                    rs_z(layer, rx, p, way).start()

    edge = jnp.logical_or(z == 0, z == nz - 1)

    @pl.loop(0, nz)
    def _(k):
        at_distance(k + 1, forward)

        @pl.when(k == 0)
        def _():
            for load in loads[:3]:
                load.wait()
            mine = ag[z, :rows, :cols]
            gate = jnp.dot(mine, sg[...], preferred_element_type=jnp.float32)
            lift = jnp.dot(mine, su[...], preferred_element_type=jnp.float32)
            hidden = (jax.nn.silu(gate) * lift).astype(jnp.bfloat16)
            shared[...] = jnp.dot(hidden, sd[...], preferred_element_type=jnp.float32)
            for load in loads[3:]:
                load.wait()

        experts_on(pick(order, k))
        at_distance(k + 1, relay)

        @pl.when(k >= 1)
        def _():
            fold_core(pick(order, k - 1))

        @pl.when(jnp.logical_and(k >= 2, edge))
        def _():
            send_sum(pick(order, k - 1))

    fold_core(pick(order, nz - 1))

    @pl.loop(0, nz - 1)
    def _(j):
        @pl.when(jnp.logical_or(jnp.logical_not(edge), j == nz - 2))
        def _():
            send_sum(pick(inner, j))

    def add_chains(p, rx):
        ds = part(p, 0, rx)
        for way in (0, 1):

            @pl.when(z > 0 if way == 0 else z < nz - 1)
            def _():
                rs_z(z, rx, p, way).wait_recv()
                keep[z, ds] = keep[z, ds] + chain[way, z, ds].astype(jnp.float32)

    for p in count:
        if pieces[p][2]:
            add_chains(p, 1)
            sx[z, part(p, 0, 0)] = local_sum(z, 1, p).astype(jnp.bfloat16)
            rs_across(z, p).start()
    for p in sorted(count, key=lambda p: pieces[p][2]):
        ds = part(p, 0, 0)
        add_chains(p, 0)
        rs_across(z, p).wait_recv()
        total = local_sum(z, 0, p) + shared[ds]
        if pieces[p][2]:
            total += rs_x[z, ds].astype(jnp.float32)
        out[ds] = total.astype(out.dtype)

    @pl.loop(0, nz)
    def _(layer):
        for p in count:
            for rx in (0, 1):
                ag_d(layer, rx, p).wait_send()
            if not pieces[p][2]:
                ag_x(layer, p).wait_send()
                rs_across(layer, p).wait_send()
            else:

                @pl.when(layer == z)
                def _():
                    ag_x(layer, p).wait_send()
                    rs_across(layer, p).wait_send()

        rs_core(layer).wait_send()
        for way in (0, 1):
            behind = layer <= z if way == 0 else layer >= z
            ahead = layer > z if way == 0 else layer < z

            @pl.when(jnp.logical_and(behind, has(way)))
            def _():
                for p, rx in kinds:
                    ag_z(layer, rx, p, way).wait_send()

            @pl.when(ahead)
            def _():
                for p, rx in kinds:
                    rs_z(layer, rx, p, way).wait_send()


def fused_shards(
    tokens,
    norm_gain,
    routes,
    gates,
    expert_gate,
    expert_up,
    expert_down,
    shared_gate,
    shared_up,
    shared_down,
):
    rows, cols = tokens.shape
    ff = expert_gate.shape[2]
    shared_ff = shared_gate.shape[1]
    ranks = lax.axis_size("ep")
    nz = ranks // 4
    pieces = make_pieces(rows)
    count = len(pieces)
    width = cols + -(-2 * ranks // 128) * 128
    half, narrow = jnp.bfloat16, pltpu.SemaphoreType.DMA
    vmem, anywhere = pl.BlockSpec(memory_space=pltpu.VMEM), pl.BlockSpec(memory_space=pl.ANY)
    return pl.pallas_call(
        functools.partial(fused_kernel, nz, pieces),
        out_shape=jax.ShapeDtypeStruct((rows, cols), half),
        in_specs=[vmem] * 4 + [anywhere] * 6,
        out_specs=vmem,
        scratch_shapes=[
            pltpu.VMEM((nz, 4 * rows, width), half),
            pltpu.VMEM((cols, ff), half),
            pltpu.VMEM((cols, ff), half),
            pltpu.VMEM((ff, cols), half),
            pltpu.VMEM((cols, shared_ff), half),
            pltpu.VMEM((cols, shared_ff), half),
            pltpu.VMEM((shared_ff, cols), half),
            pltpu.VMEM((rows, cols), jnp.float32),
            pltpu.VMEM((nz, 2 * rows, cols), jnp.float32),
            pltpu.VMEM((nz, 2 * rows, cols), half),
            pltpu.VMEM((nz, 2 * rows, cols), half),
            pltpu.VMEM((nz, rows, cols), half),
            pltpu.VMEM((nz, rows, cols), half),
            pltpu.VMEM((nz, 2 * rows, cols), half),
            pltpu.VMEM((2, nz, 2 * rows, cols), half),
            narrow((6,)),
            narrow((2, nz, 2, count)),
            narrow((nz, 2, count)),
            narrow((nz, count)),
            narrow((nz, count)),
            narrow((nz, 2, count)),
            narrow((nz, 2, count)),
            narrow((nz,)),
            narrow((nz,)),
            narrow((nz, count)),
            narrow((nz, count)),
            narrow((nz, 2, count)),
            narrow((2, nz, 2, count)),
        ],
        compiler_params=pltpu.CompilerParams(
            collective_id=0, has_side_effects=True, vmem_limit_bytes=60 * 1024 * 1024
        ),
    )(
        tokens,
        norm_gain[None, :],
        routes.T,
        gates.T,
        expert_gate[0],
        expert_up[0],
        expert_down[0],
        shared_gate,
        shared_up,
        shared_down,
    )


def make_pieces(rows):
    unit = rows // 4
    return [(i * unit, unit, i == 3) for i in range(4)]


def solution(mesh):
    in_specs = (
        P(("grp", "ep"), None),
        P(),
        P(("grp", "ep"), None),
        P(("grp", "ep"), None),
        P("ep", None, "tp"),
        P("ep", None, "tp"),
        P("ep", "tp", None),
        P(None, "tp"),
        P(None, "tp"),
        P("tp", None),
    )
    out_specs = P(("grp", "ep"), "tp")
    def body(*args):
        fits = mesh.shape["tp"] == 1 and mesh.shape["ep"] % 4 == 0 and args[4].shape[0] == 1
        small = args[0].shape[0] * mesh.shape["ep"] <= args[4].shape[1]
        return (fused_shards if fits and small else shards)(*args)

    return jax.shard_map(body, mesh=mesh, in_specs=in_specs, out_specs=out_specs, check_vma=False)
```
